768 devices in a mesh: ra: 24 (over z, core), cb: 32 (over y, x).
Axes of the slice: x: 4, y: 8, z: 12, core: 2. Of those that a mesh axis runs over, the one named last changes fastest.
Arguments:
- tokens: bfloat16 [2, 128, 3072], P(None, None, 'ra'), may hold values from -70 to 70
- norm_gain: float32 [2, 3072], P(None, 'ra'), may hold values from 0.1 to 1.9
- gate_weight: float32 [2, 3072, 8448], P(None, 'ra', 'cb'), may hold values from -0.109375 to 0.109375
- gate_scale: float32 [2, 8448], P(None, 'cb'), may hold values from 0.5 to 2
- up_weight: float32 [2, 3072, 8448], P(None, 'ra', 'cb'), may hold values from -0.109375 to 0.109375
- up_scale: float32 [2, 8448], P(None, 'cb'), may hold values from 0.5 to 2
- conv_weight: float32 [2, 3, 8448], P(None, None, 'cb'), may hold values from -3.5 to 3.5
- conv_bias: float32 [2, 8448], P(None, 'cb'), may hold values from -3 to 3
- down_weight: float32 [2, 8448, 3072], P(None, 'cb', 'ra'), may hold values from -0.0625 to 0.0625
- down_scale: float32 [2, 3072], P(None, 'ra'), may hold values from 0.5 to 2
Outputs:
- layer_output: bfloat16 [2, 128, 3072], P(None, None, 'ra')
The draws below stay inside these ranges and needn't reach their ends.
All inputs are finite; a program needn't handle non-finite values.
Results may differ from the reference program's by a relative error of at most 0.014.
Values may be sent and summed in bfloat16 or wider, within the bound.
A program may use at most 32 MiB of HBM per device.

```python
import math
import jax
import jax.numpy as jnp
from jax import lax

WIDTH = 3072
UNITS = 8448
KERNEL = 3
SEQUENCES = 2
LENGTH = 128


def draw_tokens(key, part):
    first, second, third = jax.random.split(key, 3)
    column_scale = jnp.exp(jnp.linspace(0.0, math.log(6.0), WIDTH)).astype(jnp.float32)
    rough = jnp.exp(jax.random.uniform(second, (WIDTH,), jnp.float32, -0.5, 0.5))
    row_scale = jnp.exp(jax.random.uniform(third, (SEQUENCES, LENGTH, 1), jnp.float32, 0.0, math.log(10.0)))
    base = jnp.clip(jax.random.normal(first, (SEQUENCES, LENGTH, WIDTH), jnp.float32), -4.0, 4.0)
    values = base * column_scale * rough * row_scale / 6.0
    return values.astype(jnp.bfloat16)


def shard_levels(key, shape, pieces, smallest, high):
    level, own = 1.0, jax.random.fold_in(key, 6)
    for position, shards_of in pieces:
        heights = jnp.exp(jax.random.uniform(jax.random.fold_in(own, position), (shards_of,), jnp.float32, smallest / len(pieces), high / len(pieces)))
        level = level * jnp.repeat(heights, shape[position] // shards_of).reshape([-1 if axis == position else 1 for axis in range(len(shape))])
    return level


def normal_values(rng, extent, deviation, most, pieces=(), held_as=jnp.bfloat16):
    gain = shard_levels(rng, extent, pieces, -0.22, 0.18) if pieces else 1.0
    drawn = jax.random.normal(rng, extent, jnp.float32) * deviation * gain
    return jnp.minimum(jnp.maximum(drawn, -most), most).astype(held_as)


def setup_inputs(seed: int = 0) -> dict:
    keys = jax.random.split(jax.random.key(seed), 11)
    tokens = draw_tokens(jax.random.fold_in(keys[10], 71), 0)
    norm_gain = jnp.clip(1.0 + 0.18 * jax.random.normal(keys[1], (2, WIDTH), jnp.float32), 0.1, 1.9)
    gate_weight = normal_values(keys[2], (2, WIDTH, UNITS), WIDTH ** -0.5, 0.109375, ((1, 24), (2, 32)), jnp.float32)
    gate_scale = jnp.clip(jnp.exp(math.log(2.0) - 1.3862944 * jax.random.uniform(keys[3], (2, UNITS), jnp.float32) ** shard_levels(keys[3], (2, UNITS), ((1, 32),), -0.2, 0.2)), 0.5, 2.0)
    up_weight = normal_values(keys[4], (2, WIDTH, UNITS), WIDTH ** -0.5, 0.109375, ((1, 24), (2, 32)), jnp.float32)
    up_scale = jnp.clip(jnp.exp(math.log(2.0) - 1.3862944 * jax.random.uniform(keys[5], (2, UNITS), jnp.float32) ** shard_levels(keys[5], (2, UNITS), ((1, 32),), -0.2, 0.2)), 0.5, 2.0)
    conv_weight = normal_values(keys[6], (2, KERNEL, UNITS), KERNEL ** -0.5, 3.5, ((2, 32),), jnp.float32)
    conv_bias = normal_values(keys[7], (2, UNITS), 0.5, 3.0, ((1, 32),), jnp.float32)
    down_weight = normal_values(keys[8], (2, UNITS, WIDTH), UNITS ** -0.5, 0.0625, ((1, 32), (2, 24)), jnp.float32)
    down_scale = jnp.clip(jnp.exp(math.log(2.0) - 1.3862944 * jax.random.uniform(keys[9], (2, WIDTH), jnp.float32) ** shard_levels(keys[9], (2, WIDTH), ((1, 24),), -0.2, 0.2)), 0.5, 2.0)
    return {"tokens": tokens, "norm_gain": norm_gain, "gate_weight": gate_weight, "gate_scale": gate_scale, "up_weight": up_weight, "up_scale": up_scale, "conv_weight": conv_weight, "conv_bias": conv_bias, "down_weight": down_weight, "down_scale": down_scale}


eps = 1e-06
residual_keep = 0.5

def causal_mix(gate_seq, conv_taps, conv_shift):
    count = conv_taps.shape[0]
    padded = jnp.pad(gate_seq, ((0, 0), (count - 1, 0), (0, 0)))
    running = jnp.zeros_like(gate_seq) + conv_shift[None, None, :]
    for offset in range(count):
        running = running + conv_taps[offset][None, None, :] * padded[:, offset:offset + LENGTH, :]
    return running

def sublayer(current, norm_g, gate_w, gate_s, up_w, up_s, conv_taps, conv_shift, down_w, down_s):
    values = current.astype(jnp.float32).reshape(SEQUENCES * LENGTH, WIDTH)
    inverse_rms = lax.rsqrt(lax.optimization_barrier(jnp.mean(values * values, axis=1, keepdims=True)) + eps)
    scaled = (values * norm_g[None, :]).astype(jnp.bfloat16)
    gate_sum = jnp.dot(scaled, gate_w.astype(jnp.bfloat16), preferred_element_type=jnp.float32)
    up_sum = jnp.dot(scaled, up_w.astype(jnp.bfloat16), preferred_element_type=jnp.float32)
    gate_sum = gate_sum * inverse_rms * gate_s[None, :]
    up_sum = up_sum * inverse_rms * up_s[None, :]
    conv_out = causal_mix(gate_sum.reshape(SEQUENCES, LENGTH, UNITS), conv_taps, conv_shift)
    hidden_act = (jax.nn.silu(conv_out) * up_sum.reshape(SEQUENCES, LENGTH, UNITS)).astype(jnp.bfloat16)
    hidden_act = hidden_act.reshape(SEQUENCES * LENGTH, UNITS)
    branch = jnp.dot(hidden_act, down_w.astype(jnp.bfloat16), preferred_element_type=jnp.float32) * down_s[None, :]
    return (residual_keep * values + branch).astype(jnp.bfloat16).reshape(SEQUENCES, LENGTH, WIDTH)

def reference(tokens, norm_gain, gate_weight, gate_scale, up_weight, up_scale, conv_weight, conv_bias, down_weight, down_scale):
    current = tokens
    for layer_index in range(2):
        current = sublayer(current, norm_gain[layer_index], gate_weight[layer_index], gate_scale[layer_index], up_weight[layer_index], up_scale[layer_index], conv_weight[layer_index], conv_bias[layer_index], down_weight[layer_index], down_scale[layer_index])
    return current
```

```python
import functools

import jax
import jax.numpy as jnp
from jax import lax
from jax.experimental import pallas as pl
from jax.experimental.pallas import tpu as pltpu
from jax.sharding import PartitionSpec as P

EPS = 1e-06
KEEP = 0.5
F32 = jnp.float32
BF16 = jnp.bfloat16
MESH = pl.DeviceIdType.MESH


def nt(a, b, precision=None):
    return lax.dot_general(
        a, b, (((1,), (1,)), ((), ())), preferred_element_type=F32, precision=precision
    )


def nn(a, b):
    return lax.dot_general(a, b, (((1,), (0,)), ((), ())), preferred_element_type=F32)


def ring_offsets(n):
    return sorted(range(1, n), key=lambda d: -min(d, n - d))


def plane_offsets(ny, nx):
    away = lambda p: min(p[0], ny - p[0]) + min(p[1], nx - p[1])
    return sorted(
        ((dy, dx) for dy in range(ny) for dx in range(nx) if dy or dx), key=lambda p: -away(p)
    )


def kernel(
    cfg,
    tok_h, g_h, wg_h, gs_h, wu_h, us_h, cw_h, cbias_h, wd_h, ds_h,
    out_ref,
    tok, g, wg, gs, wu, us, cw, cbias, wd, ds,
    xt_send, hT, gT, dsT, w1, w2, prm,
    s1, r1, r2, s3, r3, hn_send, fin,
    load_sem, ex_send, ex_recv, ph_send, ph_recv,
):
    NZ, NY, NX, FC, U, UP, T, width = cfg
    NB = NY * NX
    UZ = U // NZ
    FB = 2 * FC // NB
    HB = NB // 2
    ra = lax.axis_index("ra")
    cb = lax.axis_index("cb")
    z = lax.div(ra, 2)
    c = lax.rem(ra, 2)
    o = 1 - c
    y = lax.div(cb, NX)
    x = lax.rem(cb, NX)

    barrier = pltpu.get_barrier_semaphore()

    def zpeer(d):
        return (2 * lax.rem(z + d, NZ) + c, cb)

    def plane_index(off):
        return lax.rem(y + off[0], NY) * NX + lax.rem(x + off[1], NX)

    ring = ring_offsets(NZ)
    plane = plane_offsets(NY, NX)
    peers = [zpeer(d) for d in ring] + [(ra, plane_index(p)) for p in plane]
    peers += [(2 * z + o, plane_index(p)) for p in plane] + [(2 * z + o, cb)]
    for peer in peers:
        pl.semaphore_signal(barrier, inc=1, device_id=peer, device_id_type=MESH)

    pairs = [
        (tok_h, tok), (g_h, g), (wg_h, wg), (wu_h, wu), (gs_h, gs), (us_h, us),
        (cw_h, cw), (cbias_h, cbias), (wd_h, wd), (ds_h, ds),
    ]
    loads = [
        pltpu.make_async_copy(src, dst, load_sem.at[i]) for i, (src, dst) in enumerate(pairs)
    ]
    for load in loads:
        load.start()

    own_half = pl.ds(pl.multiple_of(c * FC, FC), FC)
    own_slots = pl.ds(c * HB, HB)

    def column_tile(row):
        return jnp.transpose(jnp.broadcast_to(row, (T, FC)))

    loads[0].wait()
    mine = jnp.transpose(tok[c].astype(F32)).reshape(HB, FB, T).astype(BF16)
    hT[0, own_slots] = mine
    xt_send[...] = jnp.transpose(tok[o].astype(F32)).reshape(HB, FB, T).astype(BF16)
    loads[1].wait()
    for l in range(2):
        gT[l, own_half, :] = column_tile(g[l : l + 1, :])

    row = lax.broadcasted_iota(jnp.int32, (NZ * 2 * UP, U), 0)
    col = lax.broadcasted_iota(jnp.int32, (NZ * 2 * UP, U), 1)
    block = lax.div(row, 2 * UP)
    inner = row - block * (2 * UP)
    pick_g = ((inner < UZ) & (col == block * UZ + inner)).astype(F32).astype(BF16)
    upper = inner - UP
    pick_u = (
        ((upper >= 0) & (upper < UZ) & (col == block * UZ + upper)).astype(F32).astype(BF16)
    )

    def arrange_in(l):
        w1[l, c] = (nt(pick_g, wg[l].astype(BF16)) + nt(pick_u, wu[l].astype(BF16))).astype(BF16)

    loads[2].wait()
    loads[3].wait()
    arrange_in(0)

    def to_partner(k, src, dst):
        return pltpu.make_async_remote_copy(
            src_ref=src,
            dst_ref=dst,
            send_sem=ex_send.at[k],
            recv_sem=ex_recv.at[k],
            device_id=(2 * z + o, cb),
            device_id_type=MESH,
        )

    ex = [
        to_partner(0, xt_send, hT.at[0, own_slots]),
        to_partner(1, gT.at[0, own_half, :], gT.at[0, own_half, :]),
        to_partner(2, w1.at[0, c], w1.at[0, c]),
        to_partner(3, w2.at[0, own_half, :], w2.at[0, own_half, :]),
        to_partner(4, dsT.at[:, own_half, :], dsT.at[:, own_half, :]),
        to_partner(5, gT.at[1, own_half, :], gT.at[1, own_half, :]),
        to_partner(6, w1.at[1, c], w1.at[1, c]),
        to_partner(7, w2.at[1, own_half, :], w2.at[1, own_half, :]),
    ]

    pl.semaphore_wait(barrier, len(peers))
    for k in range(3):
        ex[k].start()

    def prepare_rest():
        for k in range(4, 10):
            loads[k].wait()
        rows = [gs[0:1, :], gs[1:2, :], us[0:1, :], us[1:2, :], cbias[0:1, :], cbias[1:2, :]]
        rows += [cw[0, j : j + 1, :] for j in range(3)] + [cw[1, j : j + 1, :] for j in range(3)]
        rows += [jnp.zeros((16 - len(rows), U), F32)]
        table = jnp.concatenate(rows, axis=0)
        unit = lax.broadcasted_iota(jnp.int32, (UP, U), 0)
        at = lax.broadcasted_iota(jnp.int32, (UP, U), 1)
        own = ((unit < UZ) & (at == z * UZ + unit)).astype(F32)
        picked = nt(own, table, precision=lax.Precision.HIGHEST)
        for k in range(12):
            prm[k] = jnp.broadcast_to(picked[:, k : k + 1], (UP, T))
        for l in range(2):
            dsT[l, own_half, :] = column_tile(ds[l : l + 1, :])
        urow = lax.broadcasted_iota(jnp.int32, (NZ * UP, U), 0)
        ucol = lax.broadcasted_iota(jnp.int32, (NZ * UP, U), 1)
        ublock = lax.div(urow, UP)
        uin = urow - ublock * UP
        pick_d = ((uin < UZ) & (ucol == ublock * UZ + uin)).astype(F32).astype(BF16)
        eye = (
            lax.broadcasted_iota(jnp.int32, (FC, FC), 0)
            == lax.broadcasted_iota(jnp.int32, (FC, FC), 1)
        ).astype(F32).astype(BF16)
        for l in range(2):
            arranged = nn(pick_d, wd[l].astype(BF16)).astype(BF16)
            w2[l, own_half, :] = nt(eye, arranged).astype(BF16)
            if l == 0:
                ex[3].start()
                ex[4].start()
        arrange_in(1)
        for k in range(5, 8):
            ex[k].start()

    lane = lax.broadcasted_iota(jnp.int32, (UP, T), 1)

    def shifted(v, by):
        return jnp.where(lane >= by, pltpu.roll(v, by, 1), 0.0)

    def remote(l, p, src, dst, peer):
        return pltpu.make_async_remote_copy(
            src_ref=src,
            dst_ref=dst,
            send_sem=ph_send.at[l, p],
            recv_sem=ph_recv.at[l, p],
            device_id=peer,
            device_id_type=MESH,
        )

    def wait_bytes(sem, ref):
        pltpu.make_async_copy(ref, ref, sem).wait()

    for l in range(2):
        for k in (range(3) if l == 0 else range(5, 7)):
            ex[k].wait_recv()
        h = hT[l].astype(F32).reshape(2 * FC, T)
        squares = jnp.sum(h * h, axis=0, keepdims=True)
        scaled = (h * gT[l]).astype(BF16)
        both = jnp.concatenate([w1[l, 0], w1[l, 1]], axis=1)
        part = nn(both, scaled).reshape(NZ, 2 * UP, T)
        high = squares.astype(BF16).astype(F32)
        low = squares - high
        sub = lax.broadcasted_iota(jnp.int32, (2 * UP, T), 0)
        extra = jnp.where(sub == UZ, high, 0.0) + jnp.where(sub == UZ + 1, low, 0.0)
        part = (part + extra[None]).astype(BF16)
        s1[l] = part
        for d in ring:
            to = lax.rem(z + d, NZ)
            remote(l, 0, s1.at[l, to], r1.at[l, z], (2 * to + c, cb)).start()
        r1[l, z] = s1[l, z]
        if l == 0:
            prepare_rest()
        wait_bytes(ph_recv.at[l, 0], r1.at[l, pl.ds(0, NZ - 1)])
        total = jnp.sum(r1[l].astype(F32), axis=0)
        square_sum = total[UZ : UZ + 1, :] + total[UZ + 1 : UZ + 2, :]
        inverse_rms = lax.rsqrt(square_sum / width + EPS)
        gate = total[:UP] * inverse_rms * prm[l]
        up = total[UP:] * inverse_rms * prm[2 + l]
        taps = [prm[6 + 3 * l + j] for j in range(3)]
        conv = prm[4 + l] + taps[0] * shifted(gate, 2) + taps[1] * shifted(gate, 1) + taps[2] * gate
        hidden = (conv / (1.0 + jnp.exp(-conv))) * up
        r2[l, z] = hidden.astype(BF16)
        for d in ring:
            remote(l, 1, r2.at[l, z], r2.at[l, z], zpeer(d)).start()
        ex[3 if l == 0 else 7].wait_recv()
        if l == 0:
            ex[4].wait_recv()
        wait_bytes(ph_recv.at[l, 1], r2.at[l, pl.ds(0, NZ - 1)])
        act = r2[l].astype(F32).reshape(NZ * UP, T).astype(BF16)
        s3[l] = nn(w2[l], act).reshape(NB, FB, T).astype(BF16)
        for off in plane:
            to = plane_index(off)
            remote(l, 2, s3.at[l, to], r3.at[l, cb], (ra, to)).start()
        r3[l, cb] = s3[l, cb]
        wait_bytes(ph_recv.at[l, 2], r3.at[l, pl.ds(0, NB - 1)])
        branch = jnp.sum(r3[l].astype(F32), axis=0)
        branch = branch * dsT[l, pl.ds(pl.multiple_of(cb * FB, FB), FB), :]
        fresh = (KEEP * hT[l, cb].astype(F32) + branch).astype(BF16)
        if l == 0:
            hT[1, cb] = fresh
            for off in plane:
                remote(l, 3, hT.at[1, cb], hT.at[1, cb], (ra, plane_index(off))).start()
            wait_bytes(ph_recv.at[l, 3], hT.at[1, pl.ds(0, NB - 1)])
        else:
            half = lax.div(cb, HB)
            slot = lax.rem(cb, HB)
            owner = 2 * z + half
            hn_send[...] = fresh
            for off in plane:
                remote(l, 3, hn_send, fin.at[c, slot], (owner, plane_index(off))).start()

            @pl.when(half == c)
            def _():
                fin[c, slot] = fresh
                wait_bytes(ph_recv.at[1, 3], r3.at[0, pl.ds(0, NB - 1)])

            @pl.when(half != c)
            def _():
                remote(l, 3, hn_send, fin.at[c, slot], (owner, cb)).start()
                wait_bytes(ph_recv.at[1, 3], r3.at[0])

    out_ref[...] = fin[...]

    for copy in ex:
        copy.wait_send()
    for l in range(2):
        wait_bytes(ph_send.at[l, 0], s1.at[l, pl.ds(0, NZ - 1)])
        wait_bytes(ph_send.at[l, 1], r2.at[l, pl.ds(0, NZ - 1)])
        wait_bytes(ph_send.at[l, 2], s3.at[l, pl.ds(0, NB - 1)])
    wait_bytes(ph_send.at[0, 3], r3.at[0, pl.ds(0, NB - 1)])

    @pl.when(lax.div(cb, HB) == c)
    def _():
        wait_bytes(ph_send.at[1, 3], r3.at[0, pl.ds(0, NB - 1)])

    @pl.when(lax.div(cb, HB) != c)
    def _():
        wait_bytes(ph_send.at[1, 3], r3.at[0])


def solution(mesh, planes=(8, 4)):
    NY, NX = planes
    NZ = mesh.shape["ra"] // 2
    NB = NY * NX

    def step(*args):
        tokens, norm_gain, gate_weight = args[:3]
        _, T, FC = tokens.shape
        U = gate_weight.shape[2]
        UP = -(-(U // NZ + 2) // 8) * 8
        width = FC * mesh.shape["ra"]
        FB = 2 * FC // NB
        HB = NB // 2
        cfg = (NZ, NY, NX, FC, U, UP, T, width)
        out = pl.pallas_call(
            functools.partial(kernel, cfg),
            out_shape=jax.ShapeDtypeStruct((2, HB, FB, T), BF16),
            in_specs=[pl.BlockSpec(memory_space=pl.ANY)] * len(args),
            out_specs=pl.BlockSpec(memory_space=pltpu.VMEM),
            scratch_shapes=[pltpu.VMEM(a.shape, a.dtype) for a in args]
            + [
                pltpu.VMEM((HB, FB, T), BF16),
                pltpu.VMEM((2, NB, FB, T), BF16),
                pltpu.VMEM((2, 2 * FC, T), F32),
                pltpu.VMEM((2, 2 * FC, T), F32),
                pltpu.VMEM((2, 2, NZ * 2 * UP, FC), BF16),
                pltpu.VMEM((2, 2 * FC, NZ * UP), BF16),
                pltpu.VMEM((12, UP, T), F32),
                pltpu.VMEM((2, NZ, 2 * UP, T), BF16),
                pltpu.VMEM((2, NZ, 2 * UP, T), BF16),
                pltpu.VMEM((2, NZ, UP, T), BF16),
                pltpu.VMEM((2, NB, FB, T), BF16),
                pltpu.VMEM((2, NB, FB, T), BF16),
                pltpu.VMEM((FB, T), BF16),
                pltpu.VMEM((2, HB, FB, T), BF16),
                pltpu.SemaphoreType.DMA((len(args),)),
                pltpu.SemaphoreType.DMA((8,)),
                pltpu.SemaphoreType.DMA((8,)),
                pltpu.SemaphoreType.DMA((2, 4)),
                pltpu.SemaphoreType.DMA((2, 4)),
            ],
            compiler_params=pltpu.CompilerParams(collective_id=0, has_side_effects=True),
        )(*args)
        return jnp.transpose(out.reshape(2, FC, T), (0, 2, 1))

    in_specs = (
        P(None, None, "ra"),
        P(None, "ra"),
        P(None, "ra", "cb"),
        P(None, "cb"),
        P(None, "ra", "cb"),
        P(None, "cb"),
        P(None, None, "cb"),
        P(None, "cb"),
        P(None, "cb", "ra"),
        P(None, "ra"),
    )
    return jax.shard_map(
        step, mesh=mesh, in_specs=in_specs, out_specs=P(None, None, "ra"), check_vma=False
    )
```
